32 devices in a mesh: sp: 8 (over z, y), tp: 4 (over x, core).
Axes of the slice: x: 2, y: 2, z: 4, core: 2. Of those that a mesh axis runs over, the one named last changes fastest.
Arguments:
- tokens: bfloat16 [8192, 2048], P('sp'), may hold values from -6 to 6
- norm_gain: bfloat16 [2048], replicated, may hold values from 0.099609375 to 1.8984375
- value_proj: bfloat16 [2048, 1024], P('sp', 'tp'), may hold values from -0.125 to 0.125
- glu_proj: bfloat16 [2048, 1024], P('sp', 'tp'), may hold values from -0.125 to 0.125
- recur_proj: bfloat16 [2048, 1024], P('sp', 'tp'), may hold values from -0.125 to 0.125
- branch_proj: bfloat16 [2048, 1024], P('sp', 'tp'), may hold values from -0.125 to 0.125
- channelwise_filter_taps: bfloat16 [31, 1024], P(None, 'tp'), may hold values from -1 to 1
- group_gain: bfloat16 [1024], P('tp'), may hold values from 0.099609375 to 1.8984375
- short_kernel: bfloat16 [4, 1024], P(None, 'tp'), may hold values from -3 to 3
- decay_map: bfloat16 [16, 64, 64], P('tp'), may hold values from -0.75 to 0.75
- entry_gate_matrix: bfloat16 [16, 64, 64], P('tp'), may hold values from -0.75 to 0.75
- rate_param: float32 [1024], P('tp'), may hold values from 4.5 to 15, as said below
- extra_decay: float32 [8192, 1024], P('sp', 'tp'), may hold values from -1 to 0, as said below
- conv_out: bfloat16 [1024, 2048], P('tp', 'sp'), may hold values from -0.125 to 0.125
- recur_out: bfloat16 [1024, 2048], P('tp', 'sp'), may hold values from -0.125 to 0.125
Outputs:
- mixed: bfloat16 [8192, 2048], P(('sp', 'tp'))
The draws below stay inside these ranges and needn't reach their ends.
Inputs may be any that keep to these rules, and one draw needn't show every extreme that they name: `rate_param`: a finite parameter of each channel. `extra_decay`: every entry is negative.
All inputs are finite; a program needn't handle non-finite values.
Results may differ from the reference program's by a relative error of at most 0.015.
Values may be sent and summed in bfloat16 or wider, within the bound.
A program may use at most 64 MiB of HBM per device.

```python
import math
import jax
import jax.numpy as jnp
from jax import lax

D = 2048
CONV_CH = 1024
GROUP_CH = 64
LRU_CH = 1024
HEAD_CH = 64
KERNEL = 31
SHORT = 4
TOK_DEV = 1024
TOKENS = 8192
LRU_HEADS = 16


def draw_rate_param(key, part):
    heads = LRU_CH // HEAD_CH
    key_kind, key_slow, key_fast = jax.random.split(jax.random.fold_in(key, 11), 3)
    share = 0.5
    chooser = jax.random.uniform(key_kind, (heads,), jnp.float32) < share
    slow_kind = jnp.repeat(chooser, HEAD_CH)
    slow_rate = jnp.exp(jax.random.uniform(key_slow, (LRU_CH,), jnp.float32, math.log(0.15), math.log(0.6))) / (4.0 * TOKENS)
    fast_rate = 0.005 * jnp.exp(jax.random.uniform(key_fast, (LRU_CH,), jnp.float32, math.log(0.6), math.log(1.6)))
    rate = jnp.where(slow_kind, slow_rate, fast_rate)
    return -jnp.log(jnp.expm1(rate))


def draw_extra_decay(key, part):
    span = TOK_DEV // 4
    blocks = TOKENS // span
    heads = LRU_CH // HEAD_CH
    key_rate, key_spot, depth_random_key = jax.random.split(jax.random.fold_in(key, 23), 3)
    level = jnp.exp(jax.random.uniform(key_rate, (blocks, heads), jnp.float32, math.log(0.1), math.log(1.0))) / TOKENS
    blending_coefficient = jnp.repeat(jnp.repeat(level, span, axis=0), HEAD_CH, axis=1)
    spots_at = jax.random.randint(key_spot, (2,), 0, TOKENS)
    filter_extent = jnp.log(jax.random.uniform(depth_random_key, (2,), jnp.float32, 0.5, 0.8))
    agreement_tally = (jnp.arange(TOKENS)[:, None] == spots_at[None, :]).astype(jnp.float32)
    packet_clusters = jnp.sum(agreement_tally * filter_extent[None, :], axis=1)
    return -blending_coefficient + packet_clusters[:, None]


def steps_of(key, dims, cuts, smallest, high):
    def one(dim, parts):
        draws = jax.random.uniform(jax.random.fold_in(jax.random.fold_in(key, 6), dim), (parts,), jnp.float32, smallest / len(cuts), high / len(cuts))
        return jnp.repeat(jnp.exp(draws), dims[dim] // parts).reshape((-1,) + (1,) * (len(dims) - dim - 1))

    factor_of = one(*cuts[0])
    for cut in cuts[1:]:
        factor_of = factor_of * one(*cut)
    return factor_of


def noise(stream_key, shape, scale, most, pieces=(), held_as=jnp.bfloat16):
    entries = scale * jax.random.normal(stream_key, shape, jnp.float32)
    if pieces:
        entries = entries * steps_of(stream_key, shape, pieces, -0.22, 0.18)
    return jnp.clip(entries, -most, most).astype(held_as)


def setup_inputs(seed: int = 0) -> dict:
    keys = jax.random.split(jax.random.key(seed), 16)
    tokens = noise(keys[0], (TOKENS, D), 1.0, 6.0, ((0, 8),))
    norm_gain = jnp.clip(1.0 + 0.18 * jax.random.normal(keys[1], (D,), jnp.float32), 0.099609375, 1.8984375).astype(jnp.bfloat16)
    value_proj = noise(keys[2], (D, CONV_CH), D ** -0.5, 0.125, ((0, 8), (1, 4)))
    glu_proj = noise(keys[3], (D, CONV_CH), D ** -0.5, 0.125, ((0, 8), (1, 4)))
    recur_proj = noise(keys[4], (D, LRU_CH), D ** -0.5, 0.125, ((0, 8), (1, 4)))
    branch_proj = noise(keys[5], (D, LRU_CH), D ** -0.5, 0.125, ((0, 8), (1, 4)))
    channelwise_filter_taps = noise(keys[6], (KERNEL, CONV_CH), KERNEL ** -0.5, 1.0, ((1, 4),))
    group_gain = jnp.clip(1.0 + 0.18 * jax.random.normal(keys[7], (CONV_CH,), jnp.float32), 0.099609375, 1.8984375).astype(jnp.bfloat16)
    short_kernel = noise(keys[8], (SHORT, LRU_CH), SHORT ** -0.5, 3.0, ((1, 4),))
    decay_map = noise(keys[9], (LRU_HEADS, HEAD_CH, HEAD_CH), HEAD_CH ** -0.5, 0.75, ((0, 4),))
    entry_gate_matrix = noise(keys[10], (LRU_HEADS, HEAD_CH, HEAD_CH), HEAD_CH ** -0.5, 0.75, ((0, 4),))
    rate_param = draw_rate_param(jax.random.fold_in(keys[15], 71), 0)
    extra_decay = draw_extra_decay(jax.random.fold_in(keys[15], 71), 0)
    conv_out = noise(keys[13], (CONV_CH, D), (CONV_CH + LRU_CH) ** -0.5, 0.125, ((0, 4), (1, 8)))
    recur_out = noise(keys[14], (LRU_CH, D), (CONV_CH + LRU_CH) ** -0.5, 0.125, ((0, 4), (1, 8)))
    return dict(tokens=tokens, norm_gain=norm_gain, value_proj=value_proj, glu_proj=glu_proj, recur_proj=recur_proj, branch_proj=branch_proj, channelwise_filter_taps=channelwise_filter_taps, group_gain=group_gain, short_kernel=short_kernel, decay_map=decay_map, entry_gate_matrix=entry_gate_matrix, rate_param=rate_param, extra_decay=extra_decay, conv_out=conv_out, recur_out=recur_out)


eps = 1e-06
gate_scale = 8.0

def causal_taps(series, kernel):
    taps = kernel.shape[0]
    length = series.shape[0]
    padded = jnp.concatenate([jnp.zeros((taps - 1, series.shape[1]), jnp.float32), series], axis=0)
    total = jnp.zeros(series.shape, jnp.float32)
    for offset in range(taps):
        total = total + kernel[offset] * padded[offset:offset + length]
    return total

def merge_pair(earlier, later):
    return (earlier[0] * later[0], later[0] * earlier[1] + later[1])

def reference(tokens, norm_gain, value_proj, glu_proj, recur_proj, branch_proj, channelwise_filter_taps, group_gain, short_kernel, decay_map, entry_gate_matrix, rate_param, extra_decay, conv_out, recur_out):
    f32 = jnp.float32
    x_float = tokens.astype(f32)
    scale = lax.rsqrt(lax.optimization_barrier(jnp.mean(x_float * x_float, axis=-1, keepdims=True)) + eps)
    normed = (x_float * scale * norm_gain.astype(f32)).astype(jnp.bfloat16)
    value_part = jnp.dot(normed, value_proj, preferred_element_type=f32)
    glu_part = jnp.dot(normed, glu_proj, preferred_element_type=f32)
    arm_portion = jnp.dot(normed, branch_proj, preferred_element_type=f32)
    rec_input = jnp.dot(normed, recur_proj, preferred_element_type=f32).astype(jnp.bfloat16)
    gated = (value_part * jax.nn.sigmoid(glu_part)).astype(jnp.bfloat16)
    conv_sum = causal_taps(gated.astype(f32), channelwise_filter_taps.astype(f32))
    length = conv_sum.shape[0]
    grouped = conv_sum.reshape(length, CONV_CH // GROUP_CH, GROUP_CH)
    center = lax.optimization_barrier(jnp.mean(grouped, axis=-1, keepdims=True))
    spread = grouped - center
    var = lax.optimization_barrier(jnp.mean(spread * spread, axis=-1, keepdims=True))
    grouped = (spread * lax.rsqrt(var + eps)).reshape(length, CONV_CH)
    y_conv = jax.nn.silu(grouped * group_gain.astype(f32)).astype(jnp.bfloat16)
    rec_conv = causal_taps(rec_input.astype(f32), short_kernel.astype(f32)).astype(jnp.bfloat16)
    heads_view = rec_conv.astype(f32).reshape(length, LRU_HEADS, HEAD_CH)
    recur_gate = jax.nn.sigmoid(jnp.einsum('shi,hij->shj', heads_view, decay_map.astype(f32)).reshape(length, LRU_CH))
    input_gate = jax.nn.sigmoid(jnp.einsum('shi,hij->shj', heads_view, entry_gate_matrix.astype(f32)).reshape(length, LRU_CH))
    log_decay = -gate_scale * recur_gate * jax.nn.softplus(-rate_param)[None, :] + extra_decay
    decay = jnp.exp(log_decay)
    drive = jnp.sqrt(-jnp.expm1(2.0 * log_decay)) * input_gate * rec_conv.astype(f32)
    state = lax.associative_scan(merge_pair, (decay, drive), axis=0)[1]
    y_lru = (state * jax.nn.gelu(arm_portion, approximate=True)).astype(jnp.bfloat16)
    total = jnp.dot(y_conv, conv_out, preferred_element_type=f32) + jnp.dot(y_lru, recur_out, preferred_element_type=f32)
    return total.astype(jnp.bfloat16)
```

```python
import functools

import jax
import jax.numpy as jnp
from jax import lax
from jax.experimental import pallas as pl
from jax.experimental.pallas import tpu as pltpu
from jax.sharding import PartitionSpec as P

GROUP_CH = 64
HEAD_CH = 64
HALO = 32

eps = 1e-06
gate_scale = 8.0
f32 = jnp.float32
bf16 = jnp.bfloat16


def vmem():
    return pl.BlockSpec(memory_space=pltpu.VMEM)


def project_kernel(x_ref, gain_ref, w_ref, g_ref, r_ref, b_ref):
    x = x_ref[...].astype(f32)
    scale = lax.rsqrt(jnp.mean(x * x, axis=-1, keepdims=True) + eps)
    normed = (x * scale * gain_ref[...]).astype(bf16)
    c = g_ref.shape[1]

    def part(i):
        return jnp.dot(normed, w_ref[:, i * c : (i + 1) * c], preferred_element_type=f32)

    g_ref[...] = (part(0) * jax.nn.sigmoid(part(1))).astype(bf16).astype(f32)
    r_ref[...] = part(2).astype(bf16).astype(f32)
    b_ref[...] = jax.nn.gelu(part(3), approximate=True)


def project(tokens, gain, w, tile=256):
    rows, d = tokens.shape
    c = w.shape[1] // 4
    out = jax.ShapeDtypeStruct((rows, c), f32)
    spec = pl.BlockSpec((tile, c), lambda i: (i, 0))
    return pl.pallas_call(
        project_kernel,
        grid=(rows // tile,),
        in_specs=[
            pl.BlockSpec((tile, d), lambda i: (i, 0)),
            pl.BlockSpec((1, d), lambda i: (0, 0)),
            pl.BlockSpec(w.shape, lambda i: (0, 0)),
        ],
        out_specs=[spec] * 3,
        out_shape=[out] * 3,
        cost_estimate=pl.CostEstimate(
            flops=2 * rows * d * 4 * c, bytes_accessed=12 * 2**20, transcendentals=2 * rows * c
        ),
        name="project",
    )(tokens, gain, w)


def split_dot(x, m):
    hi = x.astype(bf16)
    rest = x - hi.astype(f32)
    mid = rest.astype(bf16)
    low = (rest - mid.astype(f32)).astype(bf16)
    dot = functools.partial(jnp.dot, preferred_element_type=f32)
    return dot(hi, m) + dot(mid, m) + dot(low, m)


def window_sum(window, taps_ref, cols, length):
    taps = taps_ref.shape[0]
    total = jnp.zeros((length, window.shape[1]), f32)
    for shift in range(8):
        offsets = [k for k in range(taps) if (HALO - taps + 1 + k) % 8 == shift]
        if not offsets:
            continue
        moved = pltpu.roll(window, window.shape[0] - shift, 0) if shift else window
        for k in offsets:
            at = HALO - taps + 1 + k - shift
            total = total + taps_ref[k : k + 1, cols] * moved[at : at + length]
    return total


def mixers_kernel(
    tile,
    g_ref,
    gh_ref,
    r_ref,
    rh_ref,
    ed_ref,
    taps_ref,
    gain_ref,
    short_ref,
    maps_ref,
    rate_ref,
    yc_ref,
    s_ref,
    a_ref,
    last_ref,
    gbuf,
    rbuf,
    cbuf,
):
    rows, c = g_ref.shape
    taps = taps_ref.shape[0]
    shorts = short_ref.shape[0]
    gbuf[0:HALO] = gh_ref[...]
    rbuf[0:HALO] = rh_ref[...]
    gbuf[HALO:] = g_ref[...]
    rbuf[HALO:] = r_ref[...]
    row_group = lax.broadcasted_iota(jnp.int32, (c, c), 0) // GROUP_CH
    col_group = lax.broadcasted_iota(jnp.int32, (c, c), 1) // GROUP_CH
    mean_map = jnp.where(row_group == col_group, 1.0 / GROUP_CH, 0.0).astype(bf16)
    sub = lax.broadcasted_iota(jnp.int32, (tile // 8, 8, c), 1)

    def step(i, carry):
        decay_in, state_in = carry
        t0 = pl.multiple_of(i * tile, tile)
        for lane in range(0, c, 128):
            cols = slice(lane, lane + 128)
            for part in range(0, tile, 64):
                cbuf[part : part + 64, cols] = window_sum(
                    gbuf[pl.ds(t0 + part, 64 + HALO), cols], taps_ref, cols, 64
                )
        x = cbuf[...]
        spread = x - split_dot(x, mean_map)
        var = split_dot(spread * spread, mean_map)
        yc_ref[pl.ds(t0, tile), :] = jax.nn.silu(
            spread * lax.rsqrt(var + eps) * gain_ref[...]
        ).astype(bf16)
        rc = window_sum(rbuf[pl.ds(t0, tile + HALO), :], short_ref, slice(None), tile)
        rc = rc.astype(bf16)
        gates = jax.nn.sigmoid(jnp.dot(rc, maps_ref[...], preferred_element_type=f32))
        log_decay = -gate_scale * gates[:, :c] * rate_ref[...] + ed_ref[pl.ds(t0, tile), :]
        y = 2.0 * log_decay
        series = jnp.full_like(y, 1.0 / 3628800.0)
        for inv in (362880.0, 40320.0, 5040.0, 720.0, 120.0, 24.0, 6.0, 2.0, 1.0):
            series = series * y + 1.0 / inv
        one_minus = jnp.where(y > -0.5, -y * series, 1.0 - jnp.exp(y))
        b = jnp.sqrt(one_minus) * gates[:, c:] * rc.astype(f32)
        a = jnp.exp(log_decay)
        a = a.reshape(tile // 8, 8, c)
        b = b.reshape(tile // 8, 8, c)
        for shift in (1, 2, 4):
            keep = sub >= shift
            a_prev = jnp.where(keep, pltpu.roll(a, shift, 1), 1.0)
            b_prev = jnp.where(keep, pltpu.roll(b, shift, 1), 0.0)
            b = b + a * b_prev
            a = a * a_prev
        for n in range(tile // 8):
            state = b[n] + a[n] * state_in
            decay = a[n] * decay_in
            s_ref[pl.ds(t0 + 8 * n, 8), :] = state
            a_ref[pl.ds(t0 + 8 * n, 8), :] = decay
            state_in = state[7:8]
            decay_in = decay[7:8]
        return decay_in, state_in

    decay, state = lax.fori_loop(
        0, rows // tile, step, (jnp.ones((1, c), f32), jnp.zeros((1, c), f32))
    )
    last_ref[0:1] = decay
    last_ref[1:2] = state


def mixers(gated, gh, rec, rh, extra, taps, gain, short, maps, rate, tile=128):
    rows, c = gated.shape
    big = jax.ShapeDtypeStruct((rows, c), f32)
    return pl.pallas_call(
        functools.partial(mixers_kernel, tile),
        in_specs=[vmem()] * 10,
        out_specs=[vmem()] * 4,
        out_shape=[
            jax.ShapeDtypeStruct((rows, c), bf16),
            big,
            big,
            jax.ShapeDtypeStruct((2, c), f32),
        ],
        scratch_shapes=[
            pltpu.VMEM((HALO + rows, c), f32),
            pltpu.VMEM((HALO + rows, c), f32),
            pltpu.VMEM((tile, c), f32),
        ],
        cost_estimate=pl.CostEstimate(
            flops=200 * rows * c * 60, bytes_accessed=8 * 2**20, transcendentals=8 * rows * c
        ),
        name="mixers",
    )(gated, gh, rec, rh, extra, taps, gain, short, maps, rate)


def output_kernel(y_ref, w_ref, o_ref):
    k = y_ref.shape[1]
    o_ref[...] = jnp.dot(
        y_ref[...], w_ref[...].reshape(k, w_ref.shape[-1]), preferred_element_type=f32
    ).astype(bf16)


def output(y, w):
    rows, k = y.shape
    sp, tp, part, cols = w.shape
    if cols % 128:
        full = jnp.transpose(w, (1, 2, 0, 3)).reshape(tp * part, sp * cols)
        return jnp.dot(y, full, preferred_element_type=f32).astype(bf16)
    return pl.pallas_call(
        output_kernel,
        grid=(sp,),
        in_specs=[
            pl.BlockSpec((rows, k), lambda j: (0, 0)),
            pl.BlockSpec((None, tp, part, cols), lambda j: (j, 0, 0, 0)),
        ],
        out_specs=pl.BlockSpec((rows, cols), lambda j: (0, j)),
        out_shape=jax.ShapeDtypeStruct((rows, sp * cols), bf16),
        name="output",
    )(y, w)


def block_diagonal(blocks):
    h, n, _ = blocks.shape
    eye = jnp.eye(h, dtype=blocks.dtype)
    return (blocks[:, :, None, :] * eye[:, None, :, None]).reshape(h * n, h * n)


def from_behind(value, axis):
    count = lax.axis_size(axis)
    return lax.ppermute(value, axis, [(s, s + 1) for s in range(count - 1)])


def body(
    tokens,
    norm_gain,
    value_proj,
    glu_proj,
    recur_proj,
    branch_proj,
    channelwise_filter_taps,
    group_gain,
    short_kernel,
    decay_map,
    entry_gate_matrix,
    rate_param,
    extra_decay,
    conv_out,
    recur_out,
):
    rows = tokens.shape[0]
    c = value_proj.shape[1]
    sp = lax.axis_size("sp")
    tp = lax.axis_size("tp")
    w_in = jnp.concatenate([value_proj, glu_proj, recur_proj, branch_proj], axis=1)
    w_in = lax.all_gather(w_in, "sp", axis=0, tiled=True)
    w_out = jnp.concatenate([conv_out, recur_out], axis=0)
    w_out = lax.all_gather(w_out, ("sp", "tp"), axis=0, tiled=False)
    w_out = w_out.reshape(sp, tp, 2 * c, conv_out.shape[1])
    gated, rec, branch = project(tokens, norm_gain.astype(f32)[None], w_in)
    tail = jnp.concatenate([gated[rows - HALO :], rec[rows - HALO :]], axis=1).astype(bf16)
    head = from_behind(tail, "sp").astype(f32)
    maps = jnp.concatenate([block_diagonal(decay_map), block_diagonal(entry_gate_matrix)], axis=1)
    y_conv, local_state, running, last = mixers(
        gated,
        head[:, :c],
        rec,
        head[:, c:],
        extra_decay,
        channelwise_filter_taps.astype(f32),
        group_gain.astype(f32)[None],
        short_kernel.astype(f32),
        maps,
        jax.nn.softplus(-rate_param)[None],
    )
    lasts = lax.all_gather(last, "sp")
    place = lax.axis_index("sp")
    incoming = jnp.zeros((c,), f32)
    for hop in range(sp - 1):
        after = lasts[hop, 0] * incoming + lasts[hop, 1]
        incoming = jnp.where(hop < place, after, incoming)
    state = local_state + running * incoming[None]
    y_lru = (state * branch).astype(bf16)
    y = jnp.concatenate([y_conv, y_lru], axis=1)
    y = lax.all_to_all(y, "tp", split_axis=0, concat_axis=1, tiled=True)
    return output(y, w_out)


def solution(mesh):
    in_specs = (
        P("sp", None),
        P(),
        P("sp", "tp"),
        P("sp", "tp"),
        P("sp", "tp"),
        P("sp", "tp"),
        P(None, "tp"),
        P("tp"),
        P(None, "tp"),
        P("tp", None, None),
        P("tp", None, None),
        P("tp"),
        P("sp", "tp"),
        P("tp", "sp"),
        P("tp", "sp"),
    )
    out_specs = P(("sp", "tp"), None)
    return jax.shard_map(body, mesh=mesh, in_specs=in_specs, out_specs=out_specs, check_vma=False)
```

```python
import functools

import jax
import jax.numpy as jnp
from jax import lax
from jax.experimental import pallas as pl
from jax.experimental.pallas import tpu as pltpu
from jax.sharding import PartitionSpec as P

GROUP_CH = 64
HEAD_CH = 64
HALO = 32

eps = 1e-06
gate_scale = 8.0
f32 = jnp.float32
bf16 = jnp.bfloat16


def vmem():
    return pl.BlockSpec(memory_space=pltpu.VMEM)


def gather_kernel(lines, width, *refs):
    count = 4
    parts, out = refs[:count], refs[count]
    send_up, recv_up, send_down, recv_down, send_side, recv_side, local = refs[count + 1 :]
    c = parts[0].shape[1]
    me = lax.axis_index("sp")
    z, y = me // width, me % width

    def signal(target):
        pl.semaphore_signal(
            barrier, inc=1, device_id={"sp": target}, device_id_type=pl.DeviceIdType.MESH
        )

    barrier = pltpu.get_barrier_semaphore()
    above, below = z < lines - 1, z > 0
    for d in (1, lines - 1) if lines > 2 else range(1, lines):
        signal((z + d) % lines * width + y)
    for d in range(1, width):
        signal(z * width + (y + d) % width)
    greeted = min(lines - 1, 2) + width - 1
    if greeted:
        pl.semaphore_wait(barrier, greeted)

    def spot(block, i):
        return out.at[block, :, pl.ds(i * c, c)]

    def remote(own, block, i, send_sem, recv_sem, target):
        return pltpu.make_async_remote_copy(
            src_ref=parts[i] if own else spot(block, i),
            dst_ref=spot(block, i),
            send_sem=send_sem,
            recv_sem=recv_sem,
            device_id={"sp": target},
            device_id_type=pl.DeviceIdType.MESH,
        )

    def up(s, i):
        return remote(
            s == 0, me - s * width, i, send_up.at[s, i], recv_up.at[s, i], me + width
        )

    def down(s, i):
        return remote(
            s == 0, me + s * width, i, send_down.at[s, i], recv_down.at[s, i], me - width
        )

    def arriving_up(s, i):
        return remote(
            False, me - s * width, i, send_up.at[s - 1, i], recv_up.at[s - 1, i], me - width
        )

    def arriving_down(s, i):
        return remote(
            False, me + s * width, i, send_down.at[s - 1, i], recv_down.at[s - 1, i], me + width
        )

    def side(s, d, i):
        slot = s + lines - 1
        target = z * width + (y + d) % width
        return remote(
            s == 0, me + s * width, i, send_side.at[slot, d - 1, i], recv_side.at[slot, d - 1, i],
            target,
        )

    def arriving_side(s, d, i):
        slot = s + lines - 1
        source = z * width + (y + width - d) % width
        return remote(
            False, source + s * width, i, send_side.at[slot, d - 1, i],
            recv_side.at[slot, d - 1, i], source,
        )

    def all_sides(s, i, act):
        for d in range(1, width):
            act(side(s, d, i))

    def start(copy):
        copy.start()

    for i in range(count):
        pl.when(above)(lambda: up(0, i).start())
        pl.when(below)(lambda: down(0, i).start())
        all_sides(0, i, start)
    own = [pltpu.make_async_copy(parts[i], spot(me, i), local.at[i]) for i in range(count)]
    for copy in own:
        copy.start()
    for s in range(1, lines):
        for i in range(count):

            @pl.when(z - s >= 0)
            def _():
                arriving_up(s, i).wait_recv()
                if s < lines - 1:
                    pl.when(above)(lambda: up(s, i).start())
                all_sides(-s, i, start)

            @pl.when(z + s < lines)
            def _():
                arriving_down(s, i).wait_recv()
                if s < lines - 1:
                    pl.when(below)(lambda: down(s, i).start())
                all_sides(s, i, start)

    for copy in own:
        copy.wait()
    for s in range(1 - lines, lines):
        for i in range(count):

            @pl.when((z + s >= 0) & (z + s < lines))
            def _():
                for d in range(1, width):
                    arriving_side(s, d, i).wait_recv()
                    side(s, d, i).wait_send()

    for s in range(lines - 1):
        for i in range(count):
            pl.when(above & (z - s >= 0))(lambda: up(s, i).wait_send())
            pl.when(below & (z + s < lines))(lambda: down(s, i).wait_send())


def gather_input(parts, lines, width):
    k, c = parts[0].shape
    dma = pltpu.SemaphoreType.DMA
    steps = max(lines - 1, 1)
    sides = (2 * lines - 1, max(width - 1, 1), 4)
    return pl.pallas_call(
        functools.partial(gather_kernel, lines, width),
        in_specs=[vmem()] * 4,
        out_specs=vmem(),
        out_shape=jax.ShapeDtypeStruct((lines * width, k, 4 * c), bf16),
        scratch_shapes=[
            dma((steps, 4)),
            dma((steps, 4)),
            dma((steps, 4)),
            dma((steps, 4)),
            dma(sides),
            dma(sides),
            dma((4,)),
        ],
        compiler_params=pltpu.CompilerParams(collective_id=0, has_side_effects=True),
        cost_estimate=pl.CostEstimate(
            flops=0, bytes_accessed=128 * 2**20, transcendentals=0
        ),
        name="gather",
    )(*parts)


def project_kernel(x_ref, gain_ref, w_ref, g_ref, r_ref, b_ref):
    x = x_ref[...].astype(f32)
    scale = lax.rsqrt(jnp.mean(x * x, axis=-1, keepdims=True) + eps)
    normed = (x * scale * gain_ref[...]).astype(bf16)
    c = g_ref.shape[1]

    def part(i):
        return jnp.dot(normed, w_ref[:, i * c : (i + 1) * c], preferred_element_type=f32)

    g_ref[...] = (part(0) * jax.nn.sigmoid(part(1))).astype(bf16).astype(f32)
    r_ref[...] = part(2).astype(bf16).astype(f32)
    b_ref[...] = jax.nn.gelu(part(3), approximate=True)


def project(tokens, gain, w, tile=256):
    rows, d = tokens.shape
    c = w.shape[1] // 4
    out = jax.ShapeDtypeStruct((rows, c), f32)
    spec = pl.BlockSpec((tile, c), lambda i: (i, 0))
    return pl.pallas_call(
        project_kernel,
        grid=(rows // tile,),
        in_specs=[
            pl.BlockSpec((tile, d), lambda i: (i, 0)),
            pl.BlockSpec((1, d), lambda i: (0, 0)),
            pl.BlockSpec(w.shape, lambda i: (0, 0)),
        ],
        out_specs=[spec] * 3,
        out_shape=[out] * 3,
        cost_estimate=pl.CostEstimate(
            flops=2 * rows * d * 4 * c, bytes_accessed=12 * 2**20, transcendentals=2 * rows * c
        ),
        name="project",
    )(tokens, gain, w)


def split_dot(x, m):
    hi = x.astype(bf16)
    rest = x - hi.astype(f32)
    mid = rest.astype(bf16)
    low = (rest - mid.astype(f32)).astype(bf16)
    dot = functools.partial(jnp.dot, preferred_element_type=f32)
    return dot(hi, m) + dot(mid, m) + dot(low, m)


def window_sum(window, taps_ref, cols, length):
    taps = taps_ref.shape[0]
    total = jnp.zeros((length, window.shape[1]), f32)
    for shift in range(8):
        offsets = [k for k in range(taps) if (HALO - taps + 1 + k) % 8 == shift]
        if not offsets:
            continue
        moved = pltpu.roll(window, window.shape[0] - shift, 0) if shift else window
        for k in offsets:
            at = HALO - taps + 1 + k - shift
            total = total + taps_ref[k : k + 1, cols] * moved[at : at + length]
    return total


def mixers_kernel(
    tile,
    g_ref,
    gh_ref,
    r_ref,
    rh_ref,
    ed_ref,
    taps_ref,
    gain_ref,
    short_ref,
    maps_ref,
    rate_ref,
    yc_ref,
    s_ref,
    a_ref,
    last_ref,
    gbuf,
    rbuf,
    cbuf,
):
    rows, c = g_ref.shape
    taps = taps_ref.shape[0]
    shorts = short_ref.shape[0]
    gbuf[0:HALO] = gh_ref[...]
    rbuf[0:HALO] = rh_ref[...]
    gbuf[HALO:] = g_ref[...]
    rbuf[HALO:] = r_ref[...]
    row_group = lax.broadcasted_iota(jnp.int32, (c, c), 0) // GROUP_CH
    col_group = lax.broadcasted_iota(jnp.int32, (c, c), 1) // GROUP_CH
    mean_map = jnp.where(row_group == col_group, 1.0 / GROUP_CH, 0.0).astype(bf16)
    sub = lax.broadcasted_iota(jnp.int32, (tile // 8, 8, c), 1)

    def step(i, carry):
        decay_in, state_in = carry
        t0 = pl.multiple_of(i * tile, tile)
        for lane in range(0, c, 128):
            cols = slice(lane, lane + 128)
            for part in range(0, tile, 64):
                cbuf[part : part + 64, cols] = window_sum(
                    gbuf[pl.ds(t0 + part, 64 + HALO), cols], taps_ref, cols, 64
                )
        x = cbuf[...]
        spread = x - split_dot(x, mean_map)
        var = split_dot(spread * spread, mean_map)
        yc_ref[pl.ds(t0, tile), :] = jax.nn.silu(
            spread * lax.rsqrt(var + eps) * gain_ref[...]
        ).astype(bf16)
        rc = window_sum(rbuf[pl.ds(t0, tile + HALO), :], short_ref, slice(None), tile)
        rc = rc.astype(bf16)
        gates = jax.nn.sigmoid(jnp.dot(rc, maps_ref[...], preferred_element_type=f32))
        log_decay = -gate_scale * gates[:, :c] * rate_ref[...] + ed_ref[pl.ds(t0, tile), :]
        y = 2.0 * log_decay
        series = jnp.full_like(y, 1.0 / 3628800.0)
        for inv in (362880.0, 40320.0, 5040.0, 720.0, 120.0, 24.0, 6.0, 2.0, 1.0):
            series = series * y + 1.0 / inv
        one_minus = jnp.where(y > -0.5, -y * series, 1.0 - jnp.exp(y))
        b = jnp.sqrt(one_minus) * gates[:, c:] * rc.astype(f32)
        a = jnp.exp(log_decay)
        a = a.reshape(tile // 8, 8, c)
        b = b.reshape(tile // 8, 8, c)
        for shift in (1, 2, 4):
            keep = sub >= shift
            a_prev = jnp.where(keep, pltpu.roll(a, shift, 1), 1.0)
            b_prev = jnp.where(keep, pltpu.roll(b, shift, 1), 0.0)
            b = b + a * b_prev
            a = a * a_prev
        for n in range(tile // 8):
            state = b[n] + a[n] * state_in
            decay = a[n] * decay_in
            s_ref[pl.ds(t0 + 8 * n, 8), :] = state
            a_ref[pl.ds(t0 + 8 * n, 8), :] = decay
            state_in = state[7:8]
            decay_in = decay[7:8]
        return decay_in, state_in

    decay, state = lax.fori_loop(
        0, rows // tile, step, (jnp.ones((1, c), f32), jnp.zeros((1, c), f32))
    )
    last_ref[0:1] = decay
    last_ref[1:2] = state


def mixers(gated, gh, rec, rh, extra, taps, gain, short, maps, rate, tile=128):
    rows, c = gated.shape
    big = jax.ShapeDtypeStruct((rows, c), f32)
    return pl.pallas_call(
        functools.partial(mixers_kernel, tile),
        in_specs=[vmem()] * 10,
        out_specs=[vmem()] * 4,
        out_shape=[
            jax.ShapeDtypeStruct((rows, c), bf16),
            big,
            big,
            jax.ShapeDtypeStruct((2, c), f32),
        ],
        scratch_shapes=[
            pltpu.VMEM((HALO + rows, c), f32),
            pltpu.VMEM((HALO + rows, c), f32),
            pltpu.VMEM((tile, c), f32),
        ],
        cost_estimate=pl.CostEstimate(
            flops=200 * rows * c * 60, bytes_accessed=8 * 2**20, transcendentals=8 * rows * c
        ),
        name="mixers",
    )(gated, gh, rec, rh, extra, taps, gain, short, maps, rate)


def output_kernel(y_ref, w_ref, o_ref):
    k = y_ref.shape[1]
    o_ref[...] = jnp.dot(
        y_ref[...], w_ref[...].reshape(k, w_ref.shape[-1]), preferred_element_type=f32
    ).astype(bf16)


def output(y, w):
    rows, k = y.shape
    sp, tp, part, cols = w.shape
    if cols % 128:
        full = jnp.transpose(w, (1, 2, 0, 3)).reshape(tp * part, sp * cols)
        return jnp.dot(y, full, preferred_element_type=f32).astype(bf16)
    return pl.pallas_call(
        output_kernel,
        grid=(sp,),
        in_specs=[
            pl.BlockSpec((rows, k), lambda j: (0, 0)),
            pl.BlockSpec((None, tp, part, cols), lambda j: (j, 0, 0, 0)),
        ],
        out_specs=pl.BlockSpec((rows, cols), lambda j: (0, j)),
        out_shape=jax.ShapeDtypeStruct((rows, sp * cols), bf16),
        name="output",
    )(y, w)


def block_diagonal(blocks):
    h, n, _ = blocks.shape
    eye = jnp.eye(h, dtype=blocks.dtype)
    return (blocks[:, :, None, :] * eye[:, None, :, None]).reshape(h * n, h * n)


def from_behind(value, axis):
    count = lax.axis_size(axis)
    return lax.ppermute(value, axis, [(s, s + 1) for s in range(count - 1)])


def body(
    tokens,
    norm_gain,
    value_proj,
    glu_proj,
    recur_proj,
    branch_proj,
    channelwise_filter_taps,
    group_gain,
    short_kernel,
    decay_map,
    entry_gate_matrix,
    rate_param,
    extra_decay,
    conv_out,
    recur_out,
):
    rows = tokens.shape[0]
    c = value_proj.shape[1]
    sp = lax.axis_size("sp")
    tp = lax.axis_size("tp")
    width = max(tp // 2, 1)
    width = width if sp % width == 0 else 1
    w_out = jnp.concatenate([conv_out, recur_out], axis=0)
    w_out = lax.all_gather(w_out, ("sp", "tp"), axis=0, tiled=False)
    w_out = w_out.reshape(sp, tp, 2 * c, conv_out.shape[1])
    w_in = gather_input([value_proj, glu_proj, recur_proj, branch_proj], sp // width, width)
    w_in = w_in.reshape(-1, 4 * c)
    gated, rec, branch = project(tokens, norm_gain.astype(f32)[None], w_in)
    tail = jnp.concatenate([gated[rows - HALO :], rec[rows - HALO :]], axis=1).astype(bf16)
    head = from_behind(tail, "sp").astype(f32)
    maps = jnp.concatenate([block_diagonal(decay_map), block_diagonal(entry_gate_matrix)], axis=1)
    y_conv, local_state, running, last = mixers(
        gated,
        head[:, :c],
        rec,
        head[:, c:],
        extra_decay,
        channelwise_filter_taps.astype(f32),
        group_gain.astype(f32)[None],
        short_kernel.astype(f32),
        maps,
        jax.nn.softplus(-rate_param)[None],
    )
    lasts = lax.all_gather(last, "sp")
    place = lax.axis_index("sp")
    incoming = jnp.zeros((c,), f32)
    for hop in range(sp - 1):
        after = lasts[hop, 0] * incoming + lasts[hop, 1]
        incoming = jnp.where(hop < place, after, incoming)
    state = local_state + running * incoming[None]
    y_lru = (state * branch).astype(bf16)
    y = jnp.concatenate([y_conv, y_lru], axis=1)
    y = lax.all_to_all(y, "tp", split_axis=0, concat_axis=1, tiled=True)
    return output(y, w_out)


def solution(mesh):
    in_specs = (
        P("sp", None),
        P(),
        P("sp", "tp"),
        P("sp", "tp"),
        P("sp", "tp"),
        P("sp", "tp"),
        P(None, "tp"),
        P("tp"),
        P(None, "tp"),
        P("tp", None, None),
        P("tp", None, None),
        P("tp"),
        P("sp", "tp"),
        P("tp", "sp"),
        P("tp", "sp"),
    )
    out_specs = P(("sp", "tp"), None)
    return jax.shard_map(body, mesh=mesh, in_specs=in_specs, out_specs=out_specs, check_vma=False)
```

```python
import functools

import jax
import jax.numpy as jnp
from jax import lax
from jax.experimental import pallas as pl
from jax.experimental.pallas import tpu as pltpu
from jax.sharding import PartitionSpec as P

GROUP_CH = 64
HEAD_CH = 64
HALO = 32

eps = 1e-06
gate_scale = 8.0
f32 = jnp.float32
bf16 = jnp.bfloat16


def vmem():
    return pl.BlockSpec(memory_space=pltpu.VMEM)


def gather_kernel(lines, width, *refs):
    count = 4
    parts, out = refs[:count], refs[count]
    send_up, recv_up, send_down, recv_down, send_side, recv_side, local = refs[count + 1 :]
    c = parts[0].shape[1]
    me = lax.axis_index("sp")
    z, y = me // width, me % width

    def signal(target):
        pl.semaphore_signal(
            barrier, inc=1, device_id={"sp": target}, device_id_type=pl.DeviceIdType.MESH
        )

    barrier = pltpu.get_barrier_semaphore()
    above, below = z < lines - 1, z > 0
    for d in (1, lines - 1) if lines > 2 else range(1, lines):
        signal((z + d) % lines * width + y)
    for d in range(1, width):
        signal(z * width + (y + d) % width)
    greeted = min(lines - 1, 2) + width - 1
    if greeted:
        pl.semaphore_wait(barrier, greeted)

    def spot(block, i):
        return out.at[block, :, pl.ds(i * c, c)]

    def remote(own, block, i, send_sem, recv_sem, target):
        return pltpu.make_async_remote_copy(
            src_ref=parts[i] if own else spot(block, i),
            dst_ref=spot(block, i),
            send_sem=send_sem,
            recv_sem=recv_sem,
            device_id={"sp": target},
            device_id_type=pl.DeviceIdType.MESH,
        )

    def up(s, i):
        return remote(
            s == 0, me - s * width, i, send_up.at[s, i], recv_up.at[s, i], me + width
        )

    def down(s, i):
        return remote(
            s == 0, me + s * width, i, send_down.at[s, i], recv_down.at[s, i], me - width
        )

    def arriving_up(s, i):
        return remote(
            False, me - s * width, i, send_up.at[s - 1, i], recv_up.at[s - 1, i], me - width
        )

    def arriving_down(s, i):
        return remote(
            False, me + s * width, i, send_down.at[s - 1, i], recv_down.at[s - 1, i], me + width
        )

    def side(s, d, i):
        slot = s + lines - 1
        target = z * width + (y + d) % width
        return remote(
            s == 0, me + s * width, i, send_side.at[slot, d - 1, i], recv_side.at[slot, d - 1, i],
            target,
        )

    def arriving_side(s, d, i):
        slot = s + lines - 1
        source = z * width + (y + width - d) % width
        return remote(
            False, source + s * width, i, send_side.at[slot, d - 1, i],
            recv_side.at[slot, d - 1, i], source,
        )

    def all_sides(s, i, act):
        for d in range(1, width):
            act(side(s, d, i))

    def start(copy):
        copy.start()

    for i in range(count):
        pl.when(above)(lambda: up(0, i).start())
        pl.when(below)(lambda: down(0, i).start())
        all_sides(0, i, start)
    own = [pltpu.make_async_copy(parts[i], spot(me, i), local.at[i]) for i in range(count)]
    for copy in own:
        copy.start()
    for s in range(1, lines):
        for i in range(count):

            @pl.when(z - s >= 0)
            def _():
                arriving_up(s, i).wait_recv()
                if s < lines - 1:
                    pl.when(above)(lambda: up(s, i).start())
                all_sides(-s, i, start)

            @pl.when(z + s < lines)
            def _():
                arriving_down(s, i).wait_recv()
                if s < lines - 1:
                    pl.when(below)(lambda: down(s, i).start())
                all_sides(s, i, start)

    for copy in own:
        copy.wait()
    for s in range(1 - lines, lines):
        for i in range(count):

            @pl.when((z + s >= 0) & (z + s < lines))
            def _():
                for d in range(1, width):
                    arriving_side(s, d, i).wait_recv()
                    side(s, d, i).wait_send()

    for s in range(lines - 1):
        for i in range(count):
            pl.when(above & (z - s >= 0))(lambda: up(s, i).wait_send())
            pl.when(below & (z + s < lines))(lambda: down(s, i).wait_send())


def gather_input(parts, lines, width):
    k, c = parts[0].shape
    dma = pltpu.SemaphoreType.DMA
    steps = max(lines - 1, 1)
    sides = (2 * lines - 1, max(width - 1, 1), 4)
    return pl.pallas_call(
        functools.partial(gather_kernel, lines, width),
        in_specs=[vmem()] * 4,
        out_specs=vmem(),
        out_shape=jax.ShapeDtypeStruct((lines * width, k, 4 * c), bf16),
        scratch_shapes=[
            dma((steps, 4)),
            dma((steps, 4)),
            dma((steps, 4)),
            dma((steps, 4)),
            dma(sides),
            dma(sides),
            dma((4,)),
        ],
        compiler_params=pltpu.CompilerParams(collective_id=0, has_side_effects=True),
        cost_estimate=pl.CostEstimate(
            flops=0, bytes_accessed=128 * 2**20, transcendentals=0
        ),
        name="gather",
    )(*parts)


def spread_kernel(count, x_ref, out_ref, send, recv, local):
    me = lax.axis_index("sp")

    def peer(d):
        return {"sp": (me + d) % count}

    barrier = pltpu.get_barrier_semaphore()
    kind = pl.DeviceIdType.MESH
    for d in range(1, count):
        pl.semaphore_signal(barrier, inc=1, device_id=peer(d), device_id_type=kind)
    pl.semaphore_wait(barrier, count - 1)
    own = pltpu.make_async_copy(x_ref, out_ref.at[me], local)
    own.start()

    def copy(d, slot):
        return pltpu.make_async_remote_copy(
            src_ref=x_ref,
            dst_ref=out_ref.at[slot],
            send_sem=send.at[d - 1],
            recv_sem=recv.at[d - 1],
            device_id=peer(d),
            device_id_type=kind,
        )

    for d in range(1, count):
        copy(d, me).start()
    own.wait()
    for d in range(1, count):
        copy(d, (me + count - d) % count).wait_recv()
        copy(d, me).wait_send()


def spread_over(x, count):
    return pl.pallas_call(
        functools.partial(spread_kernel, count),
        in_specs=[vmem()],
        out_specs=vmem(),
        out_shape=jax.ShapeDtypeStruct((count,) + x.shape, x.dtype),
        scratch_shapes=[
            pltpu.SemaphoreType.DMA((count - 1,)),
            pltpu.SemaphoreType.DMA((count - 1,)),
            pltpu.SemaphoreType.DMA,
        ],
        compiler_params=pltpu.CompilerParams(collective_id=1, has_side_effects=True),
        name="spread",
    )(x)


def project_kernel(x_ref, gain_ref, w_ref, g_ref, r_ref, b_ref):
    x = x_ref[...].astype(f32)
    scale = lax.rsqrt(jnp.mean(x * x, axis=-1, keepdims=True) + eps)
    normed = (x * scale * gain_ref[...]).astype(bf16)
    c = g_ref.shape[1]

    def part(i):
        return jnp.dot(normed, w_ref[:, i * c : (i + 1) * c], preferred_element_type=f32)

    g_ref[...] = (part(0) * jax.nn.sigmoid(part(1))).astype(bf16).astype(f32)
    r_ref[...] = part(2).astype(bf16).astype(f32)
    b_ref[...] = jax.nn.gelu(part(3), approximate=True)


def project(tokens, gain, w, tile=256):
    rows, d = tokens.shape
    c = w.shape[1] // 4
    out = jax.ShapeDtypeStruct((rows, c), f32)
    spec = pl.BlockSpec((tile, c), lambda i: (i, 0))
    return pl.pallas_call(
        project_kernel,
        grid=(rows // tile,),
        in_specs=[
            pl.BlockSpec((tile, d), lambda i: (i, 0)),
            pl.BlockSpec((1, d), lambda i: (0, 0)),
            pl.BlockSpec(w.shape, lambda i: (0, 0)),
        ],
        out_specs=[spec] * 3,
        out_shape=[out] * 3,
        cost_estimate=pl.CostEstimate(
            flops=2 * rows * d * 4 * c, bytes_accessed=12 * 2**20, transcendentals=2 * rows * c
        ),
        name="project",
    )(tokens, gain, w)


def split_dot(x, m):
    hi = x.astype(bf16)
    rest = x - hi.astype(f32)
    mid = rest.astype(bf16)
    low = (rest - mid.astype(f32)).astype(bf16)
    dot = functools.partial(jnp.dot, preferred_element_type=f32)
    return dot(hi, m) + dot(mid, m) + dot(low, m)


def window_sum(window, taps_ref, cols, length):
    taps = taps_ref.shape[0]
    total = jnp.zeros((length, window.shape[1]), f32)
    for shift in range(8):
        offsets = [k for k in range(taps) if (HALO - taps + 1 + k) % 8 == shift]
        if not offsets:
            continue
        moved = pltpu.roll(window, window.shape[0] - shift, 0) if shift else window
        for k in offsets:
            at = HALO - taps + 1 + k - shift
            total = total + taps_ref[k : k + 1, cols] * moved[at : at + length]
    return total


def mixers_kernel(
    tile,
    g_ref,
    gh_ref,
    r_ref,
    rh_ref,
    ed_ref,
    taps_ref,
    gain_ref,
    short_ref,
    maps_ref,
    rate_ref,
    yc_ref,
    s_ref,
    a_ref,
    last_ref,
    gbuf,
    rbuf,
    cbuf,
):
    rows, c = g_ref.shape
    taps = taps_ref.shape[0]
    shorts = short_ref.shape[0]
    gbuf[0:HALO] = gh_ref[...]
    rbuf[0:HALO] = rh_ref[...]
    gbuf[HALO:] = g_ref[...]
    rbuf[HALO:] = r_ref[...]
    row_group = lax.broadcasted_iota(jnp.int32, (c, c), 0) // GROUP_CH
    col_group = lax.broadcasted_iota(jnp.int32, (c, c), 1) // GROUP_CH
    mean_map = jnp.where(row_group == col_group, 1.0 / GROUP_CH, 0.0).astype(bf16)
    sub = lax.broadcasted_iota(jnp.int32, (tile // 8, 8, c), 1)

    def step(i, carry):
        decay_in, state_in = carry
        t0 = pl.multiple_of(i * tile, tile)
        for lane in range(0, c, 128):
            cols = slice(lane, lane + 128)
            for part in range(0, tile, 64):
                cbuf[part : part + 64, cols] = window_sum(
                    gbuf[pl.ds(t0 + part, 64 + HALO), cols], taps_ref, cols, 64
                )
        x = cbuf[...]
        spread = x - split_dot(x, mean_map)
        var = split_dot(spread * spread, mean_map)
        yc_ref[pl.ds(t0, tile), :] = jax.nn.silu(
            spread * lax.rsqrt(var + eps) * gain_ref[...]
        ).astype(bf16)
        rc = window_sum(rbuf[pl.ds(t0, tile + HALO), :], short_ref, slice(None), tile)
        rc = rc.astype(bf16)
        gates = jax.nn.sigmoid(jnp.dot(rc, maps_ref[...], preferred_element_type=f32))
        log_decay = -gate_scale * gates[:, :c] * rate_ref[...] + ed_ref[pl.ds(t0, tile), :]
        y = 2.0 * log_decay
        series = jnp.full_like(y, 1.0 / 3628800.0)
        for inv in (362880.0, 40320.0, 5040.0, 720.0, 120.0, 24.0, 6.0, 2.0, 1.0):
            series = series * y + 1.0 / inv
        one_minus = jnp.where(y > -0.5, -y * series, 1.0 - jnp.exp(y))
        b = jnp.sqrt(one_minus) * gates[:, c:] * rc.astype(f32)
        a = jnp.exp(log_decay)
        a = a.reshape(tile // 8, 8, c)
        b = b.reshape(tile // 8, 8, c)
        for shift in (1, 2, 4):
            keep = sub >= shift
            a_prev = jnp.where(keep, pltpu.roll(a, shift, 1), 1.0)
            b_prev = jnp.where(keep, pltpu.roll(b, shift, 1), 0.0)
            b = b + a * b_prev
            a = a * a_prev
        for n in range(tile // 8):
            state = b[n] + a[n] * state_in
            decay = a[n] * decay_in
            s_ref[pl.ds(t0 + 8 * n, 8), :] = state
            a_ref[pl.ds(t0 + 8 * n, 8), :] = decay
            state_in = state[7:8]
            decay_in = decay[7:8]
        return decay_in, state_in

    decay, state = lax.fori_loop(
        0, rows // tile, step, (jnp.ones((1, c), f32), jnp.zeros((1, c), f32))
    )
    last_ref[0:1] = decay
    last_ref[1:2] = state


def mixers(gated, gh, rec, rh, extra, taps, gain, short, maps, rate, tile=128):
    rows, c = gated.shape
    big = jax.ShapeDtypeStruct((rows, c), f32)
    return pl.pallas_call(
        functools.partial(mixers_kernel, tile),
        in_specs=[vmem()] * 10,
        out_specs=[vmem()] * 4,
        out_shape=[
            jax.ShapeDtypeStruct((rows, c), bf16),
            big,
            big,
            jax.ShapeDtypeStruct((2, c), f32),
        ],
        scratch_shapes=[
            pltpu.VMEM((HALO + rows, c), f32),
            pltpu.VMEM((HALO + rows, c), f32),
            pltpu.VMEM((tile, c), f32),
        ],
        cost_estimate=pl.CostEstimate(
            flops=200 * rows * c * 60, bytes_accessed=8 * 2**20, transcendentals=8 * rows * c
        ),
        name="mixers",
    )(gated, gh, rec, rh, extra, taps, gain, short, maps, rate)


def output_kernel(y_ref, w_ref, o_ref):
    k = y_ref.shape[1]
    o_ref[...] = jnp.dot(
        y_ref[...], w_ref[...].reshape(k, w_ref.shape[-1]), preferred_element_type=f32
    ).astype(bf16)


def output(y, w):
    rows, k = y.shape
    sp, tp, part, cols = w.shape
    if cols % 128:
        full = jnp.transpose(w, (1, 2, 0, 3)).reshape(tp * part, sp * cols)
        return jnp.dot(y, full, preferred_element_type=f32).astype(bf16)
    return pl.pallas_call(
        output_kernel,
        grid=(sp,),
        in_specs=[
            pl.BlockSpec((rows, k), lambda j: (0, 0)),
            pl.BlockSpec((None, tp, part, cols), lambda j: (j, 0, 0, 0)),
        ],
        out_specs=pl.BlockSpec((rows, cols), lambda j: (0, j)),
        out_shape=jax.ShapeDtypeStruct((rows, sp * cols), bf16),
        name="output",
    )(y, w)


def block_diagonal(blocks):
    h, n, _ = blocks.shape
    eye = jnp.eye(h, dtype=blocks.dtype)
    return (blocks[:, :, None, :] * eye[:, None, :, None]).reshape(h * n, h * n)


def from_behind(value, axis):
    count = lax.axis_size(axis)
    return lax.ppermute(value, axis, [(s, s + 1) for s in range(count - 1)])


def body(
    tokens,
    norm_gain,
    value_proj,
    glu_proj,
    recur_proj,
    branch_proj,
    channelwise_filter_taps,
    group_gain,
    short_kernel,
    decay_map,
    entry_gate_matrix,
    rate_param,
    extra_decay,
    conv_out,
    recur_out,
):
    rows = tokens.shape[0]
    c = value_proj.shape[1]
    sp = lax.axis_size("sp")
    tp = lax.axis_size("tp")
    width = max(tp // 2, 1)
    width = width if sp % width == 0 else 1
    w_out = jnp.concatenate([conv_out, recur_out], axis=0)
    w_out = lax.all_gather(w_out, ("sp", "tp"), axis=0, tiled=False)
    w_out = w_out.reshape(sp, tp, 2 * c, conv_out.shape[1])
    w_in = gather_input([value_proj, glu_proj, recur_proj, branch_proj], sp // width, width)
    w_in = w_in.reshape(-1, 4 * c)
    gated, rec, branch = project(tokens, norm_gain.astype(f32)[None], w_in)
    tail = jnp.concatenate([gated[rows - HALO :], rec[rows - HALO :]], axis=1).astype(bf16)
    head = from_behind(tail, "sp").astype(f32)
    maps = jnp.concatenate([block_diagonal(decay_map), block_diagonal(entry_gate_matrix)], axis=1)
    y_conv, local_state, running, last = mixers(
        gated,
        head[:, :c],
        rec,
        head[:, c:],
        extra_decay,
        channelwise_filter_taps.astype(f32),
        group_gain.astype(f32)[None],
        short_kernel.astype(f32),
        maps,
        jax.nn.softplus(-rate_param)[None],
    )
    lasts = spread_over(last, sp)
    place = lax.axis_index("sp")
    incoming = jnp.zeros((c,), f32)
    for hop in range(sp - 1):
        after = lasts[hop, 0] * incoming + lasts[hop, 1]
        incoming = jnp.where(hop < place, after, incoming)
    state = local_state + running * incoming[None]
    y_lru = (state * branch).astype(bf16)
    y = jnp.concatenate([y_conv, y_lru], axis=1)
    y = lax.all_to_all(y, "tp", split_axis=0, concat_axis=1, tiled=True)
    return output(y, w_out)


def solution(mesh):
    in_specs = (
        P("sp", None),
        P(),
        P("sp", "tp"),
        P("sp", "tp"),
        P("sp", "tp"),
        P("sp", "tp"),
        P(None, "tp"),
        P("tp"),
        P(None, "tp"),
        P("tp", None, None),
        P("tp", None, None),
        P("tp"),
        P("sp", "tp"),
        P("tp", "sp"),
        P("tp", "sp"),
    )
    out_specs = P(("sp", "tp"), None)
    return jax.shard_map(body, mesh=mesh, in_specs=in_specs, out_specs=out_specs, check_vma=False)
```
